32 devices in a mesh: sp: 8 (over z, y), tp: 4 (over x, core).
Axes of the slice: x: 2, y: 2, z: 4, core: 2. Of those that a mesh axis runs over, the one named last changes fastest.
Arguments:
- tokens: bfloat16 [4096, 4096], P('sp', 'tp'), may hold values from -64 to 64
- norm_gain: float32 [4096], replicated, may hold values from 0.1 to 1.9
- w_query: bfloat16 [4096, 1024], P(None, 'tp'), may hold values from -0.09375 to 0.09375
- w_key: bfloat16 [4096, 1024], P(None, 'tp'), may hold values from -0.09375 to 0.09375
- w_value: bfloat16 [4096, 1024], P(None, 'tp'), may hold values from -0.09375 to 0.09375
- w_gate_out: bfloat16 [4096, 1024], P(None, 'tp'), may hold values from -0.09375 to 0.09375
- w_gate_in: bfloat16 [4096, 1024], P(None, 'tp'), may hold values from -0.09375 to 0.09375
- w_conv_in: bfloat16 [4096, 1024], P(None, 'tp'), may hold values from -0.09375 to 0.09375
- conv_taps: float32 [3, 1024], replicated, may hold values from -3.5 to 3.5
- key_bias: bfloat16 [4096, 16], P('sp', 'tp'), may hold values from -16 to 0
- mix_gain: float32 [2048], replicated, may hold values from 0.1 to 1.9
- out_attn: bfloat16 [1024, 4096], P('tp'), may hold values from -0.125 to 0.125
- out_conv: bfloat16 [1024, 4096], P('tp'), may hold values from -0.125 to 0.125
Outputs:
- mixed: bfloat16 [4096, 4096], P('sp', 'tp')
The draws below stay inside these ranges and needn't reach their ends.
All inputs are finite; a program needn't handle non-finite values.
Results may differ from the reference program's by a relative error of at most 0.015.
Values may be sent and summed in bfloat16 or wider, within the bound.
A program may use at most 128 MiB of HBM per device.

```python
import math
import jax
import jax.numpy as jnp
from jax import lax

D = 4096
HEAD = 64
STICK_HEADS = 16
CONV_CH = 1024
CONV_WIDTH = 3
TOK_DEV = 512
SEQUENCE_LENGTH = 4096
N_SP = 8


def draw_tokens(key, part):
    key_matrix = jax.random.split(key, 3)
    base = jax.random.normal(key_matrix[0], (SEQUENCE_LENGTH, D), jnp.float32)
    ramp = jnp.exp(jnp.log(3.0) * jnp.arange(D, dtype=jnp.float32) / D)
    rough = jnp.exp(jax.random.uniform(key_matrix[1], (D,), jnp.float32, 0.0, jnp.log(10.0)))
    row_scale = jnp.exp(jax.random.uniform(key_matrix[2], (SEQUENCE_LENGTH, 1), jnp.float32, -1.0, 1.0))
    value_matrix = base * ramp * rough * row_scale / 3.0
    return jnp.clip(value_matrix, -64.0, 64.0).astype(jnp.bfloat16)


def draw_key_bias(key, part):
    key_matrix = jax.random.split(key, 7)
    fast_share = 0.5
    slow_lo = 0.1
    slow_hi = 1.4
    is_fast = jax.random.uniform(key_matrix[0], (STICK_HEADS,), jnp.float32) < fast_share
    fast_level = jax.random.uniform(key_matrix[1], (STICK_HEADS,), jnp.float32, -5.0, -3.5)
    slow_rate = jnp.exp(jax.random.uniform(key_matrix[2], (STICK_HEADS,), jnp.float32, jnp.log(slow_lo), jnp.log(slow_hi)))
    slow_level = jnp.log(slow_rate / SEQUENCE_LENGTH)
    level = jnp.where(is_fast, fast_level, slow_level)
    block_count = SEQUENCE_LENGTH // TOK_DEV
    shifts = jax.random.uniform(key_matrix[3], (block_count,), jnp.float32, -0.8, 0.8)
    per_position = jnp.repeat(shifts, TOK_DEV)
    rough = jnp.clip(0.5 * jax.random.normal(key_matrix[4], (SEQUENCE_LENGTH, STICK_HEADS), jnp.float32), -1.5, 1.5)
    spike_position = jax.random.randint(key_matrix[5], (4, STICK_HEADS), 0, SEQUENCE_LENGTH)
    match_count = jnp.any(jnp.arange(SEQUENCE_LENGTH, dtype=jnp.int32)[:, None, None] == spike_position[None], axis=1)
    portion_fraction = jax.random.uniform(key_matrix[6], (SEQUENCE_LENGTH, STICK_HEADS), jnp.float32, 0.2, 0.5)
    spike_tokens = jnp.log(portion_fraction) - jnp.log1p(-portion_fraction)
    value_matrix = level[None, :] + per_position[:, None] + rough
    return jnp.where(match_count, spike_tokens, value_matrix).astype(jnp.bfloat16)


def block_levels(rng, shape, cuts, least, top_value):
    level, own = 1.0, jax.random.fold_in(rng, 6)
    for dim, parts in cuts:
        steps = jnp.exp(jax.random.uniform(jax.random.fold_in(own, dim), (parts,), jnp.float32, least / len(cuts), top_value / len(cuts)))
        level = level * jnp.repeat(steps, shape[dim] // parts).reshape([-1 if axis == dim else 1 for axis in range(len(shape))])
    return level


def centred(own_key, dims, scale, bound, cuts=(), kind=jnp.bfloat16):
    factor_of = block_levels(own_key, dims, cuts, -0.22, 0.18) if cuts else 1.0
    values = jax.random.normal(own_key, dims, jnp.float32) * scale * factor_of
    return jnp.minimum(jnp.maximum(values, -bound), bound).astype(kind)


def setup_inputs(seed: int = 0) -> dict:
    streams_of = jax.random.split(jax.random.key(seed), 14)
    return {
        "tokens": draw_tokens(jax.random.fold_in(streams_of[13], 71), 0),
        "norm_gain": jnp.clip(1.0 + 0.18 * jax.random.normal(streams_of[1], (D,), jnp.float32), 0.1, 1.9),
        "w_query": centred(streams_of[2], (D, STICK_HEADS * HEAD), D ** -0.5, 0.09375, ((1, 4),)),
        "w_key": centred(streams_of[3], (D, STICK_HEADS * HEAD), D ** -0.5, 0.09375, ((1, 4),)),
        "w_value": centred(streams_of[4], (D, STICK_HEADS * HEAD), D ** -0.5, 0.09375, ((1, 4),)),
        "w_gate_out": centred(streams_of[5], (D, CONV_CH), D ** -0.5, 0.09375, ((1, 4),)),
        "w_gate_in": centred(streams_of[6], (D, CONV_CH), D ** -0.5, 0.09375, ((1, 4),)),
        "w_conv_in": centred(streams_of[7], (D, CONV_CH), D ** -0.5, 0.09375, ((1, 4),)),
        "conv_taps": centred(streams_of[8], (CONV_WIDTH, CONV_CH), CONV_WIDTH ** -0.5, 3.5, (), jnp.float32),
        "key_bias": draw_key_bias(jax.random.fold_in(streams_of[13], 71), 0),
        "mix_gain": jnp.clip(1.0 + 0.18 * jax.random.normal(streams_of[10], (STICK_HEADS * HEAD + CONV_CH,), jnp.float32), 0.1, 1.9),
        "out_attn": centred(streams_of[11], (STICK_HEADS * HEAD, D), (STICK_HEADS * HEAD + CONV_CH) ** -0.5, 0.125, ((0, 4),)),
        "out_conv": centred(streams_of[12], (CONV_CH, D), (STICK_HEADS * HEAD + CONV_CH) ** -0.5, 0.125, ((0, 4),)),
    }


eps = 1e-06

def stick_terms(queries, key_rows, value_rows, bias_rows, survival, causal):
    tok_rows, head_count, head_width = queries.shape
    key_count = key_rows.shape[0]
    key_span = math.gcd(key_count, 128)
    blocks = key_count // key_span
    key_heads = key_rows.reshape(key_count, head_count, head_width)
    value_heads = value_rows.reshape(key_count, head_count, head_width)
    scores = jnp.einsum('qhe,khe->hqk', queries.astype(jnp.float32), key_heads.astype(jnp.float32))
    scores = scores * head_width ** (-0.5) + jnp.transpose(bias_rows.astype(jnp.float32))[:, None, :]
    log_rest = jax.nn.log_sigmoid(-scores)
    log_take = jax.nn.log_sigmoid(scores)
    earlier = jnp.arange(key_count)[None, :] < jnp.arange(tok_rows)[:, None]
    if causal:
        log_rest = jnp.where(earlier[None], log_rest, 0.0)
    pieces = log_rest.reshape(head_count, tok_rows, blocks, key_span)
    inner = jnp.arange(key_span)
    after_mat = (inner[:, None] > inner[None, :]).astype(jnp.float32)
    within = jnp.einsum('hqbj,js->hqbs', pieces, after_mat, precision=lax.Precision.HIGHEST)
    totals = lax.optimization_barrier(jnp.sum(pieces, axis=-1))
    outer = jnp.arange(blocks)
    later_mat = (outer[:, None] > outer[None, :]).astype(jnp.float32)
    later_sum = jnp.einsum('hqb,bc->hqc', totals, later_mat, precision=lax.Precision.HIGHEST)
    after_sum = within + later_sum[..., None] + survival[:, :, None, None]
    weights = jnp.exp(log_take + after_sum.reshape(head_count, tok_rows, key_count))
    if causal:
        weights = jnp.where(earlier[None], weights, 0.0)
    weights = lax.optimization_barrier(weights.astype(jnp.bfloat16)).astype(jnp.float32)
    result = jnp.einsum('hqk,khe->qhe', weights, value_heads.astype(jnp.float32))
    return (result, survival + lax.optimization_barrier(jnp.sum(totals, axis=-1)))

def group_norm(value_matrix, gain):
    tok_rows = value_matrix.shape[0]
    grouped = value_matrix.reshape(tok_rows, -1, HEAD)
    grouped = grouped * lax.rsqrt(lax.optimization_barrier(jnp.mean(grouped * grouped, axis=-1, keepdims=True)) + eps)
    return grouped.reshape(tok_rows, -1) * gain

def reference(tokens, norm_gain, w_query, w_key, w_value, w_gate_out, w_gate_in, w_conv_in, conv_taps, key_bias, mix_gain, out_attn, out_conv):
    tok_float = tokens.astype(jnp.float32)
    row_scale = lax.rsqrt(lax.optimization_barrier(jnp.mean(tok_float * tok_float, axis=1, keepdims=True)) + eps)
    normed = (tok_float * row_scale * norm_gain).astype(jnp.bfloat16)

    def project(weight):
        return lax.optimization_barrier(jnp.dot(normed, weight, preferred_element_type=jnp.float32).astype(jnp.bfloat16))
    queries = project(w_query).reshape(SEQUENCE_LENGTH, STICK_HEADS, HEAD)
    key_rows = project(w_key)
    value_rows = project(w_value)
    zero_state = jnp.zeros((STICK_HEADS, TOK_DEV), jnp.float32)

    def attend_block(block_index):
        block_start = block_index * TOK_DEV
        own_queries = lax.dynamic_slice_in_dim(queries, block_start, TOK_DEV, 0)
        own_keys = lax.dynamic_slice_in_dim(key_rows, block_start, TOK_DEV, 0)
        own_values = lax.dynamic_slice_in_dim(value_rows, block_start, TOK_DEV, 0)
        own_bias = lax.dynamic_slice_in_dim(key_bias, block_start, TOK_DEV, 0)
        result, survival = stick_terms(own_queries, own_keys, own_values, own_bias, zero_state, True)

        def further(offset, loop_state):
            running, carried = loop_state
            key_start = (block_index - offset) * TOK_DEV
            far_keys = lax.dynamic_slice_in_dim(key_rows, key_start, TOK_DEV, 0)
            far_values = lax.dynamic_slice_in_dim(value_rows, key_start, TOK_DEV, 0)
            far_bias = lax.dynamic_slice_in_dim(key_bias, key_start, TOK_DEV, 0)
            added, carried = stick_terms(own_queries, far_keys, far_values, far_bias, carried, False)
            return (running + added, carried)
        result, survival = lax.fori_loop(jnp.int32(1), block_index + 1, further, (result, survival))
        return result
    attended = lax.map(attend_block, jnp.arange(N_SP, dtype=jnp.int32))
    attended = attended.reshape(SEQUENCE_LENGTH, STICK_HEADS * HEAD)
    gate_out = project(w_gate_out).astype(jnp.float32)
    mixed_in = project(w_gate_in).astype(jnp.float32) * project(w_conv_in).astype(jnp.float32)
    padded = jnp.pad(mixed_in, ((CONV_WIDTH - 1, 0), (0, 0)))
    convolved = jnp.zeros((SEQUENCE_LENGTH, CONV_CH), jnp.float32)
    for tap_index in range(CONV_WIDTH):
        convolved = convolved + conv_taps[tap_index] * padded[tap_index:tap_index + SEQUENCE_LENGTH]
    conv_out = gate_out * convolved
    attn_normed = group_norm(attended, mix_gain[:STICK_HEADS * HEAD]).astype(jnp.bfloat16)
    conv_normed = group_norm(conv_out, mix_gain[STICK_HEADS * HEAD:]).astype(jnp.bfloat16)
    total = jnp.dot(attn_normed, out_attn, preferred_element_type=jnp.float32)
    total = total + jnp.dot(conv_normed, out_conv, preferred_element_type=jnp.float32)
    return total.astype(jnp.bfloat16)
```

```python
import functools
import math

import jax
import jax.numpy as jnp
from jax import lax
from jax.experimental import pallas as pl
from jax.experimental.pallas import tpu as pltpu
from jax.sharding import PartitionSpec as P

HEAD = 64
STICK_HEADS = 16
CONV_WIDTH = 3
MESH = pl.DeviceIdType.MESH
LOG2E = math.log2(math.e)
SPAN = 256


eps = 1e-06


def from_behind(shard, axis, by):
    count = lax.axis_size(axis)
    pairs = [(i, i + by) for i in range(count) if 0 <= i + by < count]
    return lax.ppermute(shard, axis, pairs)


def plane_width(count):
    width = 1
    for w in range(1, count + 1):
        if count % w == 0 and w * w <= count:
            width = w
    return width


def attend_kernel(
    n,
    wide,
    q_ref,
    k_ref,
    v_ref,
    gain_ref,
    out_ref,
    kbuf,
    vbuf,
    qaug,
    tri,
    carry,
    acc,
    send_sem,
    recv_sem,
):
    rows, cols = q_ref.shape
    heads = cols // HEAD
    deep = n // wide
    me = lax.axis_index("sp")
    z, y = me // wide, me % wide

    barrier = pltpu.get_barrier_semaphore()

    def greet(cond, dev):
        @pl.when(cond)
        def _():
            pl.semaphore_signal(barrier, inc=1, device_id={"sp": dev}, device_id_type=MESH)

    greet(z > 0, me - wide)
    greet(z < deep - 1, me + wide)
    for other in range(wide):
        greet(y != other, z * wide + other)

    def copies(ksrc, vsrc, slot, m, way, dev):
        return [
            pltpu.make_async_remote_copy(
                src_ref=src,
                dst_ref=buf.at[slot],
                send_sem=send_sem.at[m, way, part],
                recv_sem=recv_sem.at[slot, part],
                device_id={"sp": dev},
                device_id_type=MESH,
            )
            for part, (src, buf) in enumerate(((ksrc, kbuf), (vsrc, vbuf)))
        ]

    def forward(ksrc, vsrc, m, act):
        slot = me - wide * m

        @pl.when(z < deep - 1)
        def _():
            for c in copies(ksrc, vsrc, slot, m, 0, me + wide):
                act(c)

        for other in range(wide):
            dev = z * wide + other

            @pl.when((y != other) & (slot < dev))
            def _():
                for c in copies(ksrc, vsrc, slot, m, 1 + other, dev):
                    act(c)

    def arrive(slot):
        for c in copies(kbuf.at[slot], vbuf.at[slot], slot, 0, 0, me):
            c.wait_recv()

    for h in range(heads):
        scaled = q_ref[:, h * HEAD : (h + 1) * HEAD].astype(jnp.float32) * (
            HEAD ** (-0.5) * LOG2E
        )
        high = scaled.astype(jnp.bfloat16)
        low = (scaled - high.astype(jnp.float32)).astype(jnp.bfloat16)
        extra = k_ref.shape[0] - cols
        lane = lax.broadcasted_iota(jnp.int32, (rows, extra), 1)
        ones = ((lane >= 2 * h) & (lane < 2 * h + 2)).astype(jnp.float32).astype(jnp.bfloat16)
        qaug[h] = jnp.concatenate([high, low, ones], axis=1)
    carry[...] = jnp.zeros_like(carry)
    acc[...] = jnp.zeros_like(acc)
    above = lax.broadcasted_iota(jnp.int32, (SPAN, SPAN), 0)
    below = lax.broadcasted_iota(jnp.int32, (SPAN, SPAN), 1)
    tri[...] = (above > below).astype(jnp.float32).astype(jnp.bfloat16)

    ends = 1 if deep > 1 else 0
    inner = (z > 0) & (z < deep - 1)

    @pl.when(inner)
    def _():
        pl.semaphore_wait(barrier, wide + 1)

    @pl.when(jnp.logical_not(inner))
    def _():
        pl.semaphore_wait(barrier, wide - 1 + ends)

    forward(k_ref, v_ref, 0, lambda c: c.start())

    def tile(q0, keys, vals, k0, diag):
        for h in range(heads):
            key = keys[h * HEAD : (h + 1) * HEAD, k0 : k0 + SPAN]
            key = jnp.concatenate([key, key, keys[cols:, k0 : k0 + SPAN]], axis=0)
            at = pl.ds(q0, SPAN)
            score = jnp.dot(qaug[h, at, :], key, preferred_element_type=jnp.float32)
            grow = jnp.exp2(jnp.minimum(score, 64.0))
            soft = jnp.maximum(score, jnp.log(1.0 + grow) * LOG2E)
            if diag:
                soft = jnp.where(below < above, soft, 0.0)
            high = soft.astype(jnp.bfloat16)
            low = (soft - high.astype(jnp.float32)).astype(jnp.bfloat16)
            cum = jnp.dot(high, tri[...], preferred_element_type=jnp.float32)
            cum = cum + jnp.dot(low, tri[...], preferred_element_type=jnp.float32)
            held = carry[h, at, :]
            after = jnp.concatenate([held] * (SPAN // 128), axis=1)
            weight = jnp.exp2((score - soft) - cum - after)
            if diag:
                weight = jnp.where(below < above, weight, 0.0)
            acc[h, at, :] += jnp.dot(
                weight.astype(jnp.bfloat16),
                vals[k0 : k0 + SPAN, h * HEAD : (h + 1) * HEAD],
                preferred_element_type=jnp.float32,
            )
            total = cum[:, :1] + soft[:, :1]
            carry[h, at, :] = held + total

    parts = rows // SPAN
    for qi in range(parts):
        for ki in reversed(range(qi + 1)):
            tile(qi * SPAN, k_ref, v_ref, ki * SPAN, qi == ki)

    def earlier(off, none):
        slot = me - off
        m = (off - 1) // wide + 1

        @pl.when(((off - 1) % wide == 0) & (me - wide * m >= 0))
        def _():
            ahead = me - wide * m
            arrive(ahead)
            forward(kbuf.at[ahead], vbuf.at[ahead], m, lambda c: c.start())

        @pl.when(off % wide != 0)
        def _():
            arrive(slot)

        @pl.loop(0, parts)
        def _(qi):
            q0 = pl.multiple_of(qi * SPAN, SPAN)
            for ki in reversed(range(parts)):
                tile(q0, kbuf.at[slot], vbuf.at[slot], ki * SPAN, False)

        return none

    lax.fori_loop(1, me + 1, earlier, 0)

    for h in range(heads):
        at = slice(h * HEAD, (h + 1) * HEAD)
        got = acc[h]
        got = got * lax.rsqrt(jnp.mean(got * got, axis=-1, keepdims=True) + eps)
        out_ref[:, at] = (got * gain_ref[:, at]).astype(out_ref.dtype)

    forward(k_ref, v_ref, 0, lambda c: c.wait_send())

    def sent(m, none):
        slot = me - wide * m
        forward(kbuf.at[slot], vbuf.at[slot], m, lambda c: c.wait_send())
        return none

    lax.fori_loop(1, z + 1, sent, 0)


def attend(queries, keys, values, gain, n):
    rows, cols = queries.shape
    heads = cols // HEAD
    wide = plane_width(n)
    depth = 2 * HEAD + keys.shape[0] - cols
    vmem = pl.BlockSpec(memory_space=pltpu.VMEM)
    return pl.pallas_call(
        functools.partial(attend_kernel, n, wide),
        name="attend",
        out_shape=jax.ShapeDtypeStruct((rows, cols), jnp.bfloat16),
        in_specs=[vmem] * 4,
        out_specs=vmem,
        scratch_shapes=[
            pltpu.VMEM((n,) + keys.shape, jnp.bfloat16),
            pltpu.VMEM((n,) + values.shape, jnp.bfloat16),
            pltpu.VMEM((heads, rows, depth), jnp.bfloat16),
            pltpu.VMEM((SPAN, SPAN), jnp.bfloat16),
            pltpu.VMEM((heads, rows, 128), jnp.float32),
            pltpu.VMEM((heads, rows, HEAD), jnp.float32),
            pltpu.SemaphoreType.DMA((n // wide, 1 + wide, 2)),
            pltpu.SemaphoreType.DMA((n, 2)),
        ],
        compiler_params=pltpu.CompilerParams(
            collective_id=0, has_side_effects=True, vmem_limit_bytes=40 * 1024 * 1024
        ),
    )(queries, keys, values, gain)


def group_norm(value_matrix, gain):
    tok_rows = value_matrix.shape[0]
    grouped = value_matrix.reshape(tok_rows, -1, HEAD)
    grouped = grouped * lax.rsqrt(jnp.mean(grouped * grouped, axis=-1, keepdims=True) + eps)
    return grouped.reshape(tok_rows, -1) * gain


def per_device(
    tokens,
    norm_gain,
    w_query,
    w_key,
    w_value,
    w_gate_out,
    w_gate_in,
    w_conv_in,
    conv_taps,
    key_bias,
    mix_gain,
    out_attn,
    out_conv,
):
    tok_rows = tokens.shape[0]
    head_cols = w_query.shape[1]
    head_count = head_cols // HEAD
    chan_count = w_conv_in.shape[1]
    tp_index = lax.axis_index("tp")
    sp_count = lax.axis_size("sp")
    gathered = lax.all_gather(tokens, "tp", axis=1, tiled=True)
    tok_float = gathered.astype(jnp.float32)
    row_scale = lax.rsqrt(jnp.mean(tok_float * tok_float, axis=1, keepdims=True) + eps)
    normed = (tok_float * row_scale * norm_gain).astype(jnp.bfloat16)

    def project(weight):
        return jnp.dot(normed, weight, preferred_element_type=jnp.float32).astype(jnp.bfloat16)

    queries = project(w_query)
    key_cols = lax.dot_general(
        w_key, normed, (((0,), (1,)), ((), ())), preferred_element_type=jnp.float32
    ).astype(jnp.bfloat16)
    value_rows = project(w_value)
    gate_out = project(w_gate_out)
    gate_in = project(w_gate_in)
    conv_in = project(w_conv_in)
    bias = jnp.transpose(key_bias.astype(jnp.float32)) * LOG2E
    bias_high = lax.reduce_precision(bias, 8, 7)
    bias_low = bias - bias_high
    extra = jnp.stack([bias_high, bias_low], axis=1).reshape(2 * head_count, tok_rows)
    extra = jnp.pad(extra, ((0, -2 * head_count % 16), (0, 0))).astype(jnp.bfloat16)
    keys = jnp.concatenate([key_cols, extra], axis=0)
    attn_gain = lax.dynamic_slice_in_dim(mix_gain, tp_index * head_cols, head_cols)
    attn_normed = attend(queries, keys, value_rows, attn_gain[None, :], sp_count)
    edge_rows = CONV_WIDTH - 1
    tail_rows = jnp.stack([gate_in[tok_rows - edge_rows :], conv_in[tok_rows - edge_rows :]])
    before = from_behind(tail_rows, "sp", 1)
    mixed_in = gate_in.astype(jnp.float32) * conv_in.astype(jnp.float32)
    earlier_mixed = before[0].astype(jnp.float32) * before[1].astype(jnp.float32)
    padded = jnp.concatenate([earlier_mixed, mixed_in], axis=0)
    own_taps = lax.dynamic_slice_in_dim(conv_taps, tp_index * chan_count, chan_count, 1)
    convolved = jnp.zeros((tok_rows, chan_count), jnp.float32)
    for tap_index in range(CONV_WIDTH):
        convolved = convolved + own_taps[tap_index] * padded[tap_index : tap_index + tok_rows]
    conv_out = gate_out.astype(jnp.float32) * convolved
    conv_gain = lax.dynamic_slice_in_dim(
        mix_gain, STICK_HEADS * HEAD + tp_index * chan_count, chan_count
    )
    conv_normed = group_norm(conv_out, conv_gain).astype(jnp.bfloat16)
    out_terms = jnp.dot(attn_normed, out_attn, preferred_element_type=jnp.float32)
    out_terms = out_terms + jnp.dot(conv_normed, out_conv, preferred_element_type=jnp.float32)
    return lax.psum_scatter(out_terms.astype(jnp.bfloat16), "tp", scatter_dimension=1, tiled=True)


def solution(mesh):
    in_specs = (
        P("sp", "tp"),
        P(),
        P(None, "tp"),
        P(None, "tp"),
        P(None, "tp"),
        P(None, "tp"),
        P(None, "tp"),
        P(None, "tp"),
        P(),
        P("sp", "tp"),
        P(),
        P("tp", None),
        P("tp", None),
    )
    out_specs = P("sp", "tp")
    return jax.shard_map(
        per_device, mesh=mesh, in_specs=in_specs, out_specs=out_specs, check_vma=False
    )
```

```python
import functools
import math

import jax
import jax.numpy as jnp
from jax import lax
from jax.experimental import pallas as pl
from jax.experimental.pallas import tpu as pltpu
from jax.sharding import PartitionSpec as P

HEAD = 64
STICK_HEADS = 16
CONV_WIDTH = 3
MESH = pl.DeviceIdType.MESH
LOG2E = math.log2(math.e)
SPAN = 256


eps = 1e-06


def from_behind(shard, axis, by):
    count = lax.axis_size(axis)
    pairs = [(i, i + by) for i in range(count) if 0 <= i + by < count]
    return lax.ppermute(shard, axis, pairs)


def plane_width(count):
    width = 1
    for w in range(1, count + 1):
        if count % w == 0 and w * w <= count:
            width = w
    return width


def attend_kernel(
    n,
    wide,
    tp,
    q_ref,
    k_ref,
    v_ref,
    gain_ref,
    conv_ref,
    wattn_ref,
    wconv_ref,
    out_ref,
    kbuf,
    vbuf,
    qaug,
    tri,
    carry,
    acc,
    wbuf,
    mixbuf,
    own_attn,
    total_ref,
    send_sem,
    recv_sem,
    wsend_sem,
    wrecv_sem,
    msend_sem,
    mrecv_sem,
):
    rows, cols = q_ref.shape
    heads = cols // HEAD
    deep = n // wide
    me = lax.axis_index("sp")
    z, y = me // wide, me % wide
    tme = lax.axis_index("tp")
    chips = tp // 2
    chip, core = tme // 2, tme % 2
    mate = chip * 2 + (1 - core)
    width = out_ref.shape[1]

    barrier = pltpu.get_barrier_semaphore()

    def greet(cond, dev):
        @pl.when(cond)
        def _():
            pl.semaphore_signal(barrier, inc=1, device_id={"sp": dev}, device_id_type=MESH)

    greet(z > 0, me - wide)
    greet(z < deep - 1, me + wide)
    for other in range(wide):
        greet(y != other, z * wide + other)

    for t in range(tp):

        @pl.when(tme != t)
        def _():
            pl.semaphore_signal(barrier, inc=1, device_id={"tp": t}, device_id_type=MESH)

    def weight_copies(t, part):
        src = (wattn_ref, wconv_ref)[part]
        return pltpu.make_async_remote_copy(
            src_ref=src.at[:, pl.ds(t * width, width)],
            dst_ref=wbuf.at[part, tme],
            send_sem=wsend_sem.at[part, t],
            recv_sem=wrecv_sem.at[part, tme],
            device_id={"tp": t},
            device_id_type=MESH,
        )

    def weight_copies_in(t, part):
        src = (wattn_ref, wconv_ref)[part]
        pltpu.make_async_remote_copy(
            src_ref=src.at[:, pl.ds(0, width)],
            dst_ref=wbuf.at[part, t],
            send_sem=wsend_sem.at[part, t],
            recv_sem=wrecv_sem.at[part, t],
            device_id={"tp": t},
            device_id_type=MESH,
        ).wait_recv()

    def own_weights(part):
        src = (wattn_ref, wconv_ref)[part]
        return pltpu.make_async_copy(
            src.at[:, pl.ds(pl.multiple_of(tme * width, width), width)],
            wbuf.at[part, tme],
            wsend_sem.at[part, tp],
        )

    def mix_copy(src, part, slot, way, dev):
        return pltpu.make_async_remote_copy(
            src_ref=src,
            dst_ref=mixbuf.at[part, slot],
            send_sem=msend_sem.at[part, way],
            recv_sem=mrecv_sem.at[part, slot],
            device_id={"tp": dev},
            device_id_type=MESH,
        )

    def spread(src, part, act):
        for other in range(chips):

            @pl.when(chip != other)
            def _():
                act(mix_copy(src, part, tme, other, other * 2 + core))

        act(mix_copy(src, part, tme, chips, mate))

    def relay(part, act):
        for other in range(chips):

            @pl.when(chip != other)
            def _():
                slot = other * 2 + core
                act(mix_copy(mixbuf.at[part, slot], part, slot, chips + 1 + other, mate))

    def arrive_relayed(part):
        for other in range(chips):

            @pl.when(chip != other)
            def _():
                slot = other * 2 + core
                mix_copy(mixbuf.at[part, slot], part, slot, 0, mate).wait_recv()

    def copies(ksrc, vsrc, slot, m, way, dev):
        return [
            pltpu.make_async_remote_copy(
                src_ref=src,
                dst_ref=buf.at[slot],
                send_sem=send_sem.at[m, way, part],
                recv_sem=recv_sem.at[slot, part],
                device_id={"sp": dev},
                device_id_type=MESH,
            )
            for part, (src, buf) in enumerate(((ksrc, kbuf), (vsrc, vbuf)))
        ]

    def forward(ksrc, vsrc, m, act):
        slot = me - wide * m

        @pl.when(z < deep - 1)
        def _():
            for c in copies(ksrc, vsrc, slot, m, 0, me + wide):
                act(c)

        for other in range(wide):
            dev = z * wide + other

            @pl.when((y != other) & (slot < dev))
            def _():
                for c in copies(ksrc, vsrc, slot, m, 1 + other, dev):
                    act(c)

    def arrive(slot):
        for c in copies(kbuf.at[slot], vbuf.at[slot], slot, 0, 0, me):
            c.wait_recv()

    for h in range(heads):
        scaled = q_ref[:, h * HEAD : (h + 1) * HEAD].astype(jnp.float32) * (
            HEAD ** (-0.5) * LOG2E
        )
        high = scaled.astype(jnp.bfloat16)
        low = (scaled - high.astype(jnp.float32)).astype(jnp.bfloat16)
        extra = k_ref.shape[0] - cols
        lane = lax.broadcasted_iota(jnp.int32, (rows, extra), 1)
        ones = ((lane >= 2 * h) & (lane < 2 * h + 2)).astype(jnp.float32).astype(jnp.bfloat16)
        qaug[h] = jnp.concatenate([high, low, ones], axis=1)
    carry[...] = jnp.zeros_like(carry)
    acc[...] = jnp.zeros_like(acc)
    above = lax.broadcasted_iota(jnp.int32, (SPAN, SPAN), 0)
    below = lax.broadcasted_iota(jnp.int32, (SPAN, SPAN), 1)
    tri[...] = (above > below).astype(jnp.float32).astype(jnp.bfloat16)

    ends = 1 if deep > 1 else 0
    inner = (z > 0) & (z < deep - 1)

    @pl.when(inner)
    def _():
        pl.semaphore_wait(barrier, wide + tp)

    @pl.when(jnp.logical_not(inner))
    def _():
        pl.semaphore_wait(barrier, wide + tp - 2 + ends)

    forward(k_ref, v_ref, 0, lambda c: c.start())
    for part in range(2):
        own_weights(part).start()
    for part in range(2):
        for t in range(tp):

            @pl.when(tme != t)
            def _():
                weight_copies(t, part).start()

    spread(conv_ref, 1, lambda c: c.start())

    def tile(q0, keys, vals, k0, diag):
        for h in range(heads):
            key = keys[h * HEAD : (h + 1) * HEAD, k0 : k0 + SPAN]
            key = jnp.concatenate([key, key, keys[cols:, k0 : k0 + SPAN]], axis=0)
            at = pl.ds(q0, SPAN)
            score = jnp.dot(qaug[h, at, :], key, preferred_element_type=jnp.float32)
            grow = jnp.exp2(jnp.minimum(score, 64.0))
            soft = jnp.maximum(score, jnp.log(1.0 + grow) * LOG2E)
            if diag:
                soft = jnp.where(below < above, soft, 0.0)
            high = soft.astype(jnp.bfloat16)
            low = (soft - high.astype(jnp.float32)).astype(jnp.bfloat16)
            cum = jnp.dot(high, tri[...], preferred_element_type=jnp.float32)
            cum = cum + jnp.dot(low, tri[...], preferred_element_type=jnp.float32)
            held = carry[h, at, :]
            after = jnp.concatenate([held] * (SPAN // 128), axis=1)
            weight = jnp.exp2((score - soft) - cum - after)
            if diag:
                weight = jnp.where(below < above, weight, 0.0)
            acc[h, at, :] += jnp.dot(
                weight.astype(jnp.bfloat16),
                vals[k0 : k0 + SPAN, h * HEAD : (h + 1) * HEAD],
                preferred_element_type=jnp.float32,
            )
            total = cum[:, :1] + soft[:, :1]
            carry[h, at, :] = held + total

    parts = rows // SPAN
    for qi in range(parts):
        for ki in reversed(range(qi + 1)):
            tile(qi * SPAN, k_ref, v_ref, ki * SPAN, qi == ki)

    def earlier(off, none):
        slot = me - off
        m = (off - 1) // wide + 1

        @pl.when(((off - 1) % wide == 0) & (me - wide * m >= 0))
        def _():
            ahead = me - wide * m
            arrive(ahead)
            forward(kbuf.at[ahead], vbuf.at[ahead], m, lambda c: c.start())

        @pl.when(off % wide != 0)
        def _():
            arrive(slot)

        @pl.loop(0, parts)
        def _(qi):
            q0 = pl.multiple_of(qi * SPAN, SPAN)
            for ki in reversed(range(parts)):
                tile(q0, kbuf.at[slot], vbuf.at[slot], ki * SPAN, False)

        return none

    lax.fori_loop(1, me + 1, earlier, 0)

    for h in range(heads):
        at = slice(h * HEAD, (h + 1) * HEAD)
        got = acc[h]
        got = got * lax.rsqrt(jnp.mean(got * got, axis=-1, keepdims=True) + eps)
        own_attn[:, at] = (got * gain_ref[:, at]).astype(own_attn.dtype)

    spread(own_attn, 0, lambda c: c.start())
    arrive_relayed(1)
    relay(1, lambda c: c.start())
    for part in range(2):
        own_weights(part).wait()
        for t in range(tp):

            @pl.when(tme != t)
            def _():
                weight_copies_in(t, part)

    mix_copy(own_attn, 0, mate, 0, mate).wait_recv()
    mix_copy(own_attn, 1, mate, 0, mate).wait_recv()
    for other in range(chips):

        @pl.when(chip != other)
        def _():
            slot = other * 2 + 1 - core
            mix_copy(own_attn, 1, slot, 0, mate).wait_recv()

    step = math.gcd(rows, 128)
    lanes = math.gcd(width, 256)

    def product(src, at, part, slot, over):
        return jnp.dot(src[at, :], wbuf[part, slot, :, over], preferred_element_type=jnp.float32)

    @pl.loop(0, rows // step)
    def _(i):
        at = pl.ds(pl.multiple_of(i * step, step), step)
        for j in range(width // lanes):
            over = slice(j * lanes, (j + 1) * lanes)
            total = product(own_attn, at, 0, tme, over)
            total += product(mixbuf.at[0, mate], at, 0, mate, over)
            total += product(conv_ref, at, 1, tme, over)
            total += product(mixbuf.at[1, mate], at, 1, mate, over)
            for k in range(1, chips):
                for c in range(2):
                    slot = (chip + k) % chips * 2 + c
                    total += product(mixbuf.at[1, slot], at, 1, slot, over)
            total_ref[at, over] = total

    arrive_relayed(0)
    relay(0, lambda c: c.start())
    for other in range(chips):

        @pl.when(chip != other)
        def _():
            slot = other * 2 + 1 - core
            mix_copy(own_attn, 0, slot, 0, mate).wait_recv()

    @pl.loop(0, rows // step)
    def _(i):
        at = pl.ds(pl.multiple_of(i * step, step), step)
        for j in range(width // lanes):
            over = slice(j * lanes, (j + 1) * lanes)
            total = total_ref[at, over]
            for k in range(1, chips):
                for c in range(2):
                    slot = (chip + k) % chips * 2 + c
                    total += product(mixbuf.at[0, slot], at, 0, slot, over)
            out_ref[at, over] = total.astype(out_ref.dtype)

    for part in range(2):
        for t in range(tp):

            @pl.when(tme != t)
            def _():
                weight_copies(t, part).wait_send()

        spread((own_attn, conv_ref)[part], part, lambda c: c.wait_send())
        relay(part, lambda c: c.wait_send())

    forward(k_ref, v_ref, 0, lambda c: c.wait_send())

    def sent(m, none):
        slot = me - wide * m
        forward(kbuf.at[slot], vbuf.at[slot], m, lambda c: c.wait_send())
        return none

    lax.fori_loop(1, z + 1, sent, 0)


def attend(queries, keys, values, gain, conv, w_attn, w_conv, n, tp):
    rows, cols = queries.shape
    heads = cols // HEAD
    wide = plane_width(n)
    width = w_attn.shape[1] // tp
    any_space = pl.BlockSpec(memory_space=pl.ANY)
    depth = 2 * HEAD + keys.shape[0] - cols
    vmem = pl.BlockSpec(memory_space=pltpu.VMEM)
    return pl.pallas_call(
        functools.partial(attend_kernel, n, wide, tp),
        name="attend",
        out_shape=jax.ShapeDtypeStruct((rows, width), jnp.bfloat16),
        in_specs=[vmem] * 5 + [any_space] * 2,
        out_specs=vmem,
        scratch_shapes=[
            pltpu.VMEM((n,) + keys.shape, jnp.bfloat16),
            pltpu.VMEM((n,) + values.shape, jnp.bfloat16),
            pltpu.VMEM((heads, rows, depth), jnp.bfloat16),
            pltpu.VMEM((SPAN, SPAN), jnp.bfloat16),
            pltpu.VMEM((heads, rows, 128), jnp.float32),
            pltpu.VMEM((heads, rows, HEAD), jnp.float32),
            pltpu.VMEM((2, tp, cols, width), jnp.bfloat16),
            pltpu.VMEM((2, tp, rows, cols), jnp.bfloat16),
            pltpu.VMEM((rows, cols), jnp.bfloat16),
            pltpu.VMEM((rows, width), jnp.float32),
            pltpu.SemaphoreType.DMA((n // wide, 1 + wide, 2)),
            pltpu.SemaphoreType.DMA((n, 2)),
            pltpu.SemaphoreType.DMA((2, tp + 1)),
            pltpu.SemaphoreType.DMA((2, tp)),
            pltpu.SemaphoreType.DMA((2, tp + 1)),
            pltpu.SemaphoreType.DMA((2, tp)),
        ],
        compiler_params=pltpu.CompilerParams(
            collective_id=0, has_side_effects=True, vmem_limit_bytes=40 * 1024 * 1024
        ),
    )(queries, keys, values, gain, conv, w_attn, w_conv)


def group_norm(value_matrix, gain):
    tok_rows = value_matrix.shape[0]
    grouped = value_matrix.reshape(tok_rows, -1, HEAD)
    grouped = grouped * lax.rsqrt(jnp.mean(grouped * grouped, axis=-1, keepdims=True) + eps)
    return grouped.reshape(tok_rows, -1) * gain


def per_device(
    tokens,
    norm_gain,
    w_query,
    w_key,
    w_value,
    w_gate_out,
    w_gate_in,
    w_conv_in,
    conv_taps,
    key_bias,
    mix_gain,
    out_attn,
    out_conv,
):
    tok_rows = tokens.shape[0]
    head_cols = w_query.shape[1]
    head_count = head_cols // HEAD
    chan_count = w_conv_in.shape[1]
    tp_index = lax.axis_index("tp")
    sp_count = lax.axis_size("sp")
    gathered = lax.all_gather(tokens, "tp", axis=1, tiled=True)
    tok_float = gathered.astype(jnp.float32)
    row_scale = lax.rsqrt(jnp.mean(tok_float * tok_float, axis=1, keepdims=True) + eps)
    normed = (tok_float * row_scale * norm_gain).astype(jnp.bfloat16)

    def project(weight):
        return jnp.dot(normed, weight, preferred_element_type=jnp.float32).astype(jnp.bfloat16)

    queries = project(w_query)
    key_cols = lax.dot_general(
        w_key, normed, (((0,), (1,)), ((), ())), preferred_element_type=jnp.float32
    ).astype(jnp.bfloat16)
    value_rows = project(w_value)
    gate_out = project(w_gate_out)
    gate_in = project(w_gate_in)
    conv_in = project(w_conv_in)
    bias = jnp.transpose(key_bias.astype(jnp.float32)) * LOG2E
    bias_high = lax.reduce_precision(bias, 8, 7)
    bias_low = bias - bias_high
    extra = jnp.stack([bias_high, bias_low], axis=1).reshape(2 * head_count, tok_rows)
    extra = jnp.pad(extra, ((0, -2 * head_count % 16), (0, 0))).astype(jnp.bfloat16)
    keys = jnp.concatenate([key_cols, extra], axis=0)
    attn_gain = lax.dynamic_slice_in_dim(mix_gain, tp_index * head_cols, head_cols)
    edge_rows = CONV_WIDTH - 1
    tail_rows = jnp.stack([gate_in[tok_rows - edge_rows :], conv_in[tok_rows - edge_rows :]])
    before = from_behind(tail_rows, "sp", 1)
    mixed_in = gate_in.astype(jnp.float32) * conv_in.astype(jnp.float32)
    earlier_mixed = before[0].astype(jnp.float32) * before[1].astype(jnp.float32)
    padded = jnp.concatenate([earlier_mixed, mixed_in], axis=0)
    own_taps = lax.dynamic_slice_in_dim(conv_taps, tp_index * chan_count, chan_count, 1)
    convolved = jnp.zeros((tok_rows, chan_count), jnp.float32)
    for tap_index in range(CONV_WIDTH):
        convolved = convolved + own_taps[tap_index] * padded[tap_index : tap_index + tok_rows]
    conv_out = gate_out.astype(jnp.float32) * convolved
    conv_gain = lax.dynamic_slice_in_dim(
        mix_gain, STICK_HEADS * HEAD + tp_index * chan_count, chan_count
    )
    conv_normed = group_norm(conv_out, conv_gain).astype(jnp.bfloat16)
    return attend(
        queries,
        keys,
        value_rows,
        attn_gain[None, :],
        conv_normed,
        out_attn,
        out_conv,
        sp_count,
        lax.axis_size("tp"),
    )


def solution(mesh):
    in_specs = (
        P("sp", "tp"),
        P(),
        P(None, "tp"),
        P(None, "tp"),
        P(None, "tp"),
        P(None, "tp"),
        P(None, "tp"),
        P(None, "tp"),
        P(),
        P("sp", "tp"),
        P(),
        P("tp", None),
        P("tp", None),
    )
    out_specs = P("sp", "tp")
    return jax.shard_map(
        per_device, mesh=mesh, in_specs=in_specs, out_specs=out_specs, check_vma=False
    )
```

```python
import functools
import math

import jax
import jax.numpy as jnp
from jax import lax
from jax.experimental import pallas as pl
from jax.experimental.pallas import tpu as pltpu
from jax.sharding import PartitionSpec as P

HEAD = 64
STICK_HEADS = 16
CONV_WIDTH = 3
MESH = pl.DeviceIdType.MESH
LOG2E = math.log2(math.e)
SPAN = 256


eps = 1e-06


def from_behind(shard, axis, by):
    count = lax.axis_size(axis)
    pairs = [(i, i + by) for i in range(count) if 0 <= i + by < count]
    return lax.ppermute(shard, axis, pairs)


def plane_width(count):
    width = 1
    for w in range(1, count + 1):
        if count % w == 0 and w * w <= count:
            width = w
    return width


def attend_kernel(
    n,
    wide,
    tp,
    q_ref,
    k_ref,
    v_ref,
    gain_ref,
    conv_ref,
    wattn_ref,
    wconv_ref,
    out_ref,
    kbuf,
    vbuf,
    qaug,
    tri,
    carry,
    acc,
    wbuf,
    mixbuf,
    own_attn,
    total_ref,
    send_sem,
    recv_sem,
    wsend_sem,
    wrecv_sem,
    msend_sem,
    mrecv_sem,
):
    rows, cols = q_ref.shape
    heads = cols // HEAD
    deep = n // wide
    me = lax.axis_index("sp")
    z, y = me // wide, me % wide
    tme = lax.axis_index("tp")
    chips = tp // 2
    chip, core = tme // 2, tme % 2
    mate = chip * 2 + (1 - core)
    width = out_ref.shape[1]

    barrier = pltpu.get_barrier_semaphore()

    def greet(cond, dev):
        @pl.when(cond)
        def _():
            pl.semaphore_signal(barrier, inc=1, device_id={"sp": dev}, device_id_type=MESH)

    greet(z > 0, me - wide)
    greet(z < deep - 1, me + wide)
    for other in range(wide):
        greet(y != other, z * wide + other)

    for t in range(tp):

        @pl.when(tme != t)
        def _():
            pl.semaphore_signal(barrier, inc=1, device_id={"tp": t}, device_id_type=MESH)

    def weight_copies(t, part):
        src = (wattn_ref, wconv_ref)[part]
        return pltpu.make_async_remote_copy(
            src_ref=src.at[:, pl.ds(t * width, width)],
            dst_ref=wbuf.at[part, tme],
            send_sem=wsend_sem.at[part, t],
            recv_sem=wrecv_sem.at[part, tme],
            device_id={"tp": t},
            device_id_type=MESH,
        )

    def weight_copies_in(t, part):
        src = (wattn_ref, wconv_ref)[part]
        pltpu.make_async_remote_copy(
            src_ref=src.at[:, pl.ds(0, width)],
            dst_ref=wbuf.at[part, t],
            send_sem=wsend_sem.at[part, t],
            recv_sem=wrecv_sem.at[part, t],
            device_id={"tp": t},
            device_id_type=MESH,
        ).wait_recv()

    def own_weights(part):
        src = (wattn_ref, wconv_ref)[part]
        return pltpu.make_async_copy(
            src.at[:, pl.ds(pl.multiple_of(tme * width, width), width)],
            wbuf.at[part, tme],
            wsend_sem.at[part, tp],
        )

    def mix_copy(src, part, slot, way, dev):
        return pltpu.make_async_remote_copy(
            src_ref=src,
            dst_ref=mixbuf.at[part, slot],
            send_sem=msend_sem.at[part, way],
            recv_sem=mrecv_sem.at[part, slot],
            device_id={"tp": dev},
            device_id_type=MESH,
        )

    def spread(src, part, act):
        for other in range(chips):

            @pl.when(chip != other)
            def _():
                act(mix_copy(src, part, tme, other, other * 2 + core))

        act(mix_copy(src, part, tme, chips, mate))

    def relay(part, act):
        for other in range(chips):

            @pl.when(chip != other)
            def _():
                slot = other * 2 + core
                act(mix_copy(mixbuf.at[part, slot], part, slot, chips + 1 + other, mate))

    def arrive_relayed(part):
        for other in range(chips):

            @pl.when(chip != other)
            def _():
                slot = other * 2 + core
                mix_copy(mixbuf.at[part, slot], part, slot, 0, mate).wait_recv()

    def copies(ksrc, vsrc, slot, m, way, dev):
        return [
            pltpu.make_async_remote_copy(
                src_ref=src,
                dst_ref=buf.at[slot],
                send_sem=send_sem.at[m, way, part],
                recv_sem=recv_sem.at[slot, part],
                device_id={"sp": dev},
                device_id_type=MESH,
            )
            for part, (src, buf) in enumerate(((ksrc, kbuf), (vsrc, vbuf)))
        ]

    def forward(ksrc, vsrc, m, act):
        slot = me - wide * m

        @pl.when(z < deep - 1)
        def _():
            for c in copies(ksrc, vsrc, slot, m, 0, me + wide):
                act(c)

        for other in range(wide):
            dev = z * wide + other

            @pl.when((y != other) & (slot < dev))
            def _():
                for c in copies(ksrc, vsrc, slot, m, 1 + other, dev):
                    act(c)

    def arrive(slot):
        for c in copies(kbuf.at[slot], vbuf.at[slot], slot, 0, 0, me):
            c.wait_recv()

    for h in range(heads):
        scaled = q_ref[:, h * HEAD : (h + 1) * HEAD].astype(jnp.float32) * (
            HEAD ** (-0.5) * LOG2E
        )
        high = scaled.astype(jnp.bfloat16)
        low = (scaled - high.astype(jnp.float32)).astype(jnp.bfloat16)
        extra = k_ref.shape[0] - cols
        lane = lax.broadcasted_iota(jnp.int32, (rows, extra), 1)
        ones = ((lane >= 2 * h) & (lane < 2 * h + 2)).astype(jnp.float32).astype(jnp.bfloat16)
        qaug[h] = jnp.concatenate([high, low, ones], axis=1)
    carry[...] = jnp.zeros_like(carry)
    acc[...] = jnp.zeros_like(acc)
    above = lax.broadcasted_iota(jnp.int32, (SPAN, SPAN), 0)
    below = lax.broadcasted_iota(jnp.int32, (SPAN, SPAN), 1)
    tri[...] = (above > below).astype(jnp.float32).astype(jnp.bfloat16)

    ends = 1 if deep > 1 else 0
    inner = (z > 0) & (z < deep - 1)

    @pl.when(inner)
    def _():
        pl.semaphore_wait(barrier, wide + tp)

    @pl.when(jnp.logical_not(inner))
    def _():
        pl.semaphore_wait(barrier, wide + tp - 2 + ends)

    forward(k_ref, v_ref, 0, lambda c: c.start())
    for part in range(2):
        own_weights(part).start()
    for part in range(2):
        for t in range(tp):

            @pl.when(tme != t)
            def _():
                weight_copies(t, part).start()

    spread(conv_ref, 1, lambda c: c.start())

    def tile(q0, keys, vals, k0, diag):
        for h in range(heads):
            key = keys[h * HEAD : (h + 1) * HEAD, k0 : k0 + SPAN]
            key = jnp.concatenate([key, key, keys[cols:, k0 : k0 + SPAN]], axis=0)
            at = pl.ds(q0, SPAN)
            score = jnp.dot(qaug[h, at, :], key, preferred_element_type=jnp.float32)
            grow = jnp.exp2(jnp.minimum(score, 64.0))
            soft = jnp.maximum(score, jnp.log(1.0 + grow) * LOG2E)
            if diag:
                soft = jnp.where(below < above, soft, 0.0)
            high = soft.astype(jnp.bfloat16)
            low = (soft - high.astype(jnp.float32)).astype(jnp.bfloat16)
            cum = jnp.dot(high, tri[...], preferred_element_type=jnp.float32)
            cum = cum + jnp.dot(low, tri[...], preferred_element_type=jnp.float32)
            held = carry[h, at, :]
            after = jnp.concatenate([held] * (SPAN // 128), axis=1)
            weight = jnp.exp2((score - soft) - cum - after)
            if diag:
                weight = jnp.where(below < above, weight, 0.0)
            acc[h, at, :] += jnp.dot(
                weight.astype(jnp.bfloat16),
                vals[k0 : k0 + SPAN, h * HEAD : (h + 1) * HEAD],
                preferred_element_type=jnp.float32,
            )
            total = cum[:, :1] + soft[:, :1]
            carry[h, at, :] = held + total

    parts = rows // SPAN
    for qi in range(parts):
        for ki in reversed(range(qi + 1)):
            tile(qi * SPAN, k_ref, v_ref, ki * SPAN, qi == ki)

    def earlier(off, none):
        slot = me - off
        m = (off - 1) // wide + 1

        @pl.when(((off - 1) % wide == 0) & (me - wide * m >= 0))
        def _():
            ahead = me - wide * m
            arrive(ahead)
            forward(kbuf.at[ahead], vbuf.at[ahead], m, lambda c: c.start())

        @pl.when(off % wide != 0)
        def _():
            arrive(slot)

        @pl.loop(0, parts)
        def _(qi):
            q0 = pl.multiple_of(qi * SPAN, SPAN)
            for ki in reversed(range(parts)):
                tile(q0, kbuf.at[slot], vbuf.at[slot], ki * SPAN, False)

        return none

    lax.fori_loop(1, me + 1, earlier, 0)

    for h in range(heads):
        at = slice(h * HEAD, (h + 1) * HEAD)
        got = acc[h]
        got = got * lax.rsqrt(jnp.mean(got * got, axis=-1, keepdims=True) + eps)
        own_attn[:, at] = (got * gain_ref[:, at]).astype(own_attn.dtype)

    spread(own_attn, 0, lambda c: c.start())
    arrive_relayed(1)
    relay(1, lambda c: c.start())
    for part in range(2):
        own_weights(part).wait()
        for t in range(tp):

            @pl.when(tme != t)
            def _():
                weight_copies_in(t, part)

    mix_copy(own_attn, 0, mate, 0, mate).wait_recv()
    mix_copy(own_attn, 1, mate, 0, mate).wait_recv()
    for other in range(chips):

        @pl.when(chip != other)
        def _():
            slot = other * 2 + 1 - core
            mix_copy(own_attn, 1, slot, 0, mate).wait_recv()

    step = math.gcd(rows, 128)
    lanes = math.gcd(width, 256)

    def product(src, at, part, slot, over):
        return jnp.dot(src[at, :], wbuf[part, slot, :, over], preferred_element_type=jnp.float32)

    @pl.loop(0, rows // step)
    def _(i):
        at = pl.ds(pl.multiple_of(i * step, step), step)
        for j in range(width // lanes):
            over = slice(j * lanes, (j + 1) * lanes)
            total = product(own_attn, at, 0, tme, over)
            total += product(mixbuf.at[0, mate], at, 0, mate, over)
            total += product(conv_ref, at, 1, tme, over)
            total += product(mixbuf.at[1, mate], at, 1, mate, over)
            for k in range(1, chips):
                for c in range(2):
                    slot = (chip + k) % chips * 2 + c
                    total += product(mixbuf.at[1, slot], at, 1, slot, over)
            total_ref[at, over] = total

    arrive_relayed(0)
    relay(0, lambda c: c.start())
    for other in range(chips):

        @pl.when(chip != other)
        def _():
            slot = other * 2 + 1 - core
            mix_copy(own_attn, 0, slot, 0, mate).wait_recv()

    @pl.loop(0, rows // step)
    def _(i):
        at = pl.ds(pl.multiple_of(i * step, step), step)
        for j in range(width // lanes):
            over = slice(j * lanes, (j + 1) * lanes)
            total = total_ref[at, over]
            for k in range(1, chips):
                for c in range(2):
                    slot = (chip + k) % chips * 2 + c
                    total += product(mixbuf.at[0, slot], at, 0, slot, over)
            out_ref[at, over] = total.astype(out_ref.dtype)

    for part in range(2):
        for t in range(tp):

            @pl.when(tme != t)
            def _():
                weight_copies(t, part).wait_send()

        spread((own_attn, conv_ref)[part], part, lambda c: c.wait_send())
        relay(part, lambda c: c.wait_send())

    forward(k_ref, v_ref, 0, lambda c: c.wait_send())

    def sent(m, none):
        slot = me - wide * m
        forward(kbuf.at[slot], vbuf.at[slot], m, lambda c: c.wait_send())
        return none

    lax.fori_loop(1, z + 1, sent, 0)


def attend(queries, keys, values, gain, conv, w_attn, w_conv, n, tp):
    rows, cols = queries.shape
    heads = cols // HEAD
    wide = plane_width(n)
    width = w_attn.shape[1] // tp
    any_space = pl.BlockSpec(memory_space=pl.ANY)
    depth = 2 * HEAD + keys.shape[0] - cols
    vmem = pl.BlockSpec(memory_space=pltpu.VMEM)
    return pl.pallas_call(
        functools.partial(attend_kernel, n, wide, tp),
        name="attend",
        out_shape=jax.ShapeDtypeStruct((rows, width), jnp.bfloat16),
        in_specs=[vmem] * 5 + [any_space] * 2,
        out_specs=vmem,
        scratch_shapes=[
            pltpu.VMEM((n,) + keys.shape, jnp.bfloat16),
            pltpu.VMEM((n,) + values.shape, jnp.bfloat16),
            pltpu.VMEM((heads, rows, depth), jnp.bfloat16),
            pltpu.VMEM((SPAN, SPAN), jnp.bfloat16),
            pltpu.VMEM((heads, rows, 128), jnp.float32),
            pltpu.VMEM((heads, rows, HEAD), jnp.float32),
            pltpu.VMEM((2, tp, cols, width), jnp.bfloat16),
            pltpu.VMEM((2, tp, rows, cols), jnp.bfloat16),
            pltpu.VMEM((rows, cols), jnp.bfloat16),
            pltpu.VMEM((rows, width), jnp.float32),
            pltpu.SemaphoreType.DMA((n // wide, 1 + wide, 2)),
            pltpu.SemaphoreType.DMA((n, 2)),
            pltpu.SemaphoreType.DMA((2, tp + 1)),
            pltpu.SemaphoreType.DMA((2, tp)),
            pltpu.SemaphoreType.DMA((2, tp + 1)),
            pltpu.SemaphoreType.DMA((2, tp)),
        ],
        compiler_params=pltpu.CompilerParams(
            collective_id=0, has_side_effects=True, vmem_limit_bytes=40 * 1024 * 1024
        ),
    )(queries, keys, values, gain, conv, w_attn, w_conv)


def project_kernel(
    tp,
    tok_ref,
    gain_ref,
    extra_ref,
    *refs,
):
    weights, outs = refs[:6], refs[6:12]
    tokbuf, wbuf, nbuf, load_sem, send_sem, recv_sem = refs[12:]
    rows, width = tok_ref.shape
    tme = lax.axis_index("tp")
    chips = tp // 2
    chip, core = tme // 2, tme % 2
    mate = chip * 2 + (1 - core)
    cut = math.gcd(rows, 128)
    steps = rows // cut

    barrier = pltpu.get_barrier_semaphore()
    for t in range(tp):

        @pl.when(tme != t)
        def _():
            pl.semaphore_signal(barrier, inc=1, device_id={"tp": t}, device_id_type=MESH)

    loads = [pltpu.make_async_copy(w, wbuf.at[i], load_sem.at[i]) for i, w in enumerate(weights)]
    pl.semaphore_wait(barrier, tp - 1)

    def copy(src, r, slot, way, dev):
        at = pl.ds(pl.multiple_of(r * cut, cut), cut)
        return pltpu.make_async_remote_copy(
            src_ref=src.at[at, :],
            dst_ref=tokbuf.at[slot, at, :],
            send_sem=send_sem.at[r, way],
            recv_sem=recv_sem.at[r, slot],
            device_id={"tp": dev},
            device_id_type=MESH,
        )

    def spread(r, act):
        for other in range(chips):

            @pl.when(chip != other)
            def _():
                act(copy(tok_ref, r, tme, other, other * 2 + core))

        act(copy(tok_ref, r, tme, chips, mate))

    def relay(r, act):
        for other in range(chips):

            @pl.when(chip != other)
            def _():
                slot = other * 2 + core
                act(copy(tokbuf.at[slot], r, slot, chips + 1 + other, mate))

    @pl.loop(0, steps)
    def _(r):
        spread(r, lambda c: c.start())

    for load in loads:
        load.start()
    tokbuf[tme] = tok_ref[...]
    for load in loads:
        load.wait()
    keys = outs[1]
    cols = outs[0].shape[1]
    keys[cols:, :] = extra_ref[...]

    for r in range(steps):
        for other in range(chips):

            @pl.when(chip != other)
            def _():
                slot = other * 2 + core
                copy(tok_ref, r, slot, 0, mate).wait_recv()

        relay(r, lambda c: c.start())
        copy(tok_ref, r, mate, 0, mate).wait_recv()
        for other in range(chips):

            @pl.when(chip != other)
            def _():
                slot = other * 2 + 1 - core
                copy(tok_ref, r, slot, 0, mate).wait_recv()

        at = slice(r * cut, (r + 1) * cut)
        square = jnp.zeros((cut, 128), jnp.float32)
        for t in range(tp):
            piece = tokbuf[t, at, :].astype(jnp.float32)
            piece = piece * piece
            for i in range(width // 128):
                square += piece[:, i * 128 : (i + 1) * 128]
        scale = lax.rsqrt(jnp.sum(square, axis=1, keepdims=True) / (tp * width) + eps)
        for t in range(tp):
            over = slice(t * width, (t + 1) * width)
            piece = tokbuf[t, at, :].astype(jnp.float32) * scale * gain_ref[:, over]
            nbuf[:, over] = piece.astype(nbuf.dtype)
        for i, out in enumerate(outs):
            got = jnp.dot(nbuf[...], wbuf[i], preferred_element_type=jnp.float32)
            if i == 1:
                out[:cols, at] = got.T.astype(out.dtype)
            else:
                out[at, :] = got.astype(out.dtype)

    @pl.loop(0, steps)
    def _(r):
        spread(r, lambda c: c.wait_send())
        relay(r, lambda c: c.wait_send())


def project_all(tokens, gain, extra, weights, tp):
    rows, width = tokens.shape
    deep, cols = weights[0].shape
    steps = rows // math.gcd(rows, 128)
    vmem = pl.BlockSpec(memory_space=pltpu.VMEM)
    flat = jax.ShapeDtypeStruct((rows, cols), jnp.bfloat16)
    turned = jax.ShapeDtypeStruct((cols + extra.shape[0], rows), jnp.bfloat16)
    return pl.pallas_call(
        functools.partial(project_kernel, tp),
        name="front",
        out_shape=(flat, turned, flat, flat, flat, flat),
        in_specs=[vmem] * 3 + [pl.BlockSpec(memory_space=pl.ANY)] * 6,
        out_specs=(vmem,) * 6,
        scratch_shapes=[
            pltpu.VMEM((tp, rows, width), jnp.bfloat16),
            pltpu.VMEM((6, deep, cols), jnp.bfloat16),
            pltpu.VMEM((rows // steps, deep), jnp.bfloat16),
            pltpu.SemaphoreType.DMA((6,)),
            pltpu.SemaphoreType.DMA((steps, tp + 1)),
            pltpu.SemaphoreType.DMA((steps, tp)),
        ],
        compiler_params=pltpu.CompilerParams(
            collective_id=1, has_side_effects=True, vmem_limit_bytes=40 * 1024 * 1024
        ),
    )(tokens, gain, extra, *weights)


def group_norm(value_matrix, gain):
    tok_rows = value_matrix.shape[0]
    grouped = value_matrix.reshape(tok_rows, -1, HEAD)
    grouped = grouped * lax.rsqrt(jnp.mean(grouped * grouped, axis=-1, keepdims=True) + eps)
    return grouped.reshape(tok_rows, -1) * gain


def per_device(
    tokens,
    norm_gain,
    w_query,
    w_key,
    w_value,
    w_gate_out,
    w_gate_in,
    w_conv_in,
    conv_taps,
    key_bias,
    mix_gain,
    out_attn,
    out_conv,
):
    tok_rows = tokens.shape[0]
    head_cols = w_query.shape[1]
    head_count = head_cols // HEAD
    chan_count = w_conv_in.shape[1]
    tp_index = lax.axis_index("tp")
    sp_count = lax.axis_size("sp")
    bias = jnp.transpose(key_bias.astype(jnp.float32)) * LOG2E
    bias_high = lax.reduce_precision(bias, 8, 7)
    bias_low = bias - bias_high
    extra = jnp.stack([bias_high, bias_low], axis=1).reshape(2 * head_count, tok_rows)
    extra = jnp.pad(extra, ((0, -2 * head_count % 16), (0, 0))).astype(jnp.bfloat16)
    queries, keys, value_rows, gate_out, gate_in, conv_in = project_all(
        tokens,
        norm_gain[None, :],
        extra,
        (w_query, w_key, w_value, w_gate_out, w_gate_in, w_conv_in),
        lax.axis_size("tp"),
    )
    attn_gain = lax.dynamic_slice_in_dim(mix_gain, tp_index * head_cols, head_cols)
    edge_rows = CONV_WIDTH - 1
    tail_rows = jnp.stack([gate_in[tok_rows - edge_rows :], conv_in[tok_rows - edge_rows :]])
    before = from_behind(tail_rows, "sp", 1)
    mixed_in = gate_in.astype(jnp.float32) * conv_in.astype(jnp.float32)
    earlier_mixed = before[0].astype(jnp.float32) * before[1].astype(jnp.float32)
    padded = jnp.concatenate([earlier_mixed, mixed_in], axis=0)
    own_taps = lax.dynamic_slice_in_dim(conv_taps, tp_index * chan_count, chan_count, 1)
    convolved = jnp.zeros((tok_rows, chan_count), jnp.float32)
    for tap_index in range(CONV_WIDTH):
        convolved = convolved + own_taps[tap_index] * padded[tap_index : tap_index + tok_rows]
    conv_out = gate_out.astype(jnp.float32) * convolved
    conv_gain = lax.dynamic_slice_in_dim(
        mix_gain, STICK_HEADS * HEAD + tp_index * chan_count, chan_count
    )
    conv_normed = group_norm(conv_out, conv_gain).astype(jnp.bfloat16)
    return attend(
        queries,
        keys,
        value_rows,
        attn_gain[None, :],
        conv_normed,
        out_attn,
        out_conv,
        sp_count,
        lax.axis_size("tp"),
    )


def solution(mesh):
    in_specs = (
        P("sp", "tp"),
        P(),
        P(None, "tp"),
        P(None, "tp"),
        P(None, "tp"),
        P(None, "tp"),
        P(None, "tp"),
        P(None, "tp"),
        P(),
        P("sp", "tp"),
        P(),
        P("tp", None),
        P("tp", None),
    )
    out_specs = P("sp", "tp")
    return jax.shard_map(
        per_device, mesh=mesh, in_specs=in_specs, out_specs=out_specs, check_vma=False
    )
```
